512 devices in a mesh: kv: 64 (over z, y), tp: 8 (over x, core).
Axes of the slice: x: 4, y: 8, z: 8, core: 2. Of those that a mesh axis runs over, the one named last changes fastest.
Arguments:
- hidden_in: bfloat16 [8, 1024], P(None, 'tp'), may hold values from -18 to 18, as said below
- input_gain: float32 [1024], P('tp'), may hold values from 0.1 to 1.9
- down_query: bfloat16 [1024, 256], P('tp'), may hold values from -0.1875 to 0.1875
- down_latent: bfloat16 [1024, 256], P('tp'), may hold values from -0.1875 to 0.1875
- down_rope: bfloat16 [1024, 64], P('tp'), may hold values from -0.1875 to 0.1875
- query_gain: float32 [256], replicated, may hold values from 0.1 to 1.9
- latent_gain: float32 [256], replicated, may hold values from 0.1 to 1.9
- up_query: bfloat16 [256, 8, 128], P(None, 'tp'), may hold values from -0.375 to 0.375
- up_rope: bfloat16 [256, 8, 64], P(None, 'tp'), may hold values from -0.375 to 0.375
- key_up: bfloat16 [256, 8, 128], P(None, 'tp'), may hold values from -0.375 to 0.375
- value_up: bfloat16 [256, 8, 128], P(None, 'tp'), may hold values from -0.375 to 0.375
- out_proj: bfloat16 [1024, 1024], P('tp', 'kv'), may hold values from -2 to 2, as said below
- output_gain: float32 [1024], P('kv'), may hold values from 0.1 to 1.9
- latent_cache: bfloat16 [8, 65536, 256], P(None, ('kv', 'tp')), may hold values from -6 to 6
- rope_cache: bfloat16 [8, 65536, 64], P(None, ('kv', 'tp')), may hold values from -6 to 6
- lengths: int32 [8], replicated, may hold values from 1 to 65536, as said below
Outputs:
- mixed: bfloat16 [8, 1024], P(None, 'kv')
The draws below stay inside these ranges and needn't reach their ends.
Inputs may be any that keep to these rules, and one draw needn't show every extreme that they name: Each length lies between 1 and 65536; in every draw some sequence has exactly 65536 and some exactly 1; lengths are heavily skewed toward short ones. `hidden_in`: activations whose size differs strongly between blocks of 64 features, by sequence. `out_proj`: output projection whose columns differ strongly in size.
All inputs are finite; a program needn't handle non-finite values.
Results may differ from the reference program's by a relative error of at most 0.015.
Values may be sent and summed in bfloat16 or wider, within the bound.
A program may use at most 128 MiB of HBM per device.

```python
import math
import jax
import jax.numpy as jnp
from jax import lax

D = 1024
H = 8
DN = 128
DR = 64
DV = 128
QR = 256
KR = 256
SEQS = 8
LEN = 65536


def draw_lengths(key, part):
    subkeys = jax.random.split(key, 3)
    drawn = jax.random.randint(subkeys[0], (SEQS,), 1, LEN + 1)
    shifts = jax.random.randint(subkeys[1], (SEQS,), 0, LEN.bit_length())
    result = jnp.maximum(jnp.right_shift(drawn, shifts), 1)
    chosen = jax.random.randint(subkeys[2], (), 0, SEQS)
    result = result.at[chosen].set(LEN)
    result = result.at[(chosen + 1) % SEQS].set(1)
    return result.astype(jnp.int32)


def draw_hidden_in(key, part):
    subkeys = jax.random.split(jax.random.fold_in(key, 11), 2)
    blocks = D // 64
    base = jnp.clip(jax.random.normal(subkeys[0], (SEQS, blocks, 64), jnp.float32), -4.0, 4.0)
    spread = jnp.exp(jax.random.uniform(subkeys[1], (SEQS, blocks, 1), jnp.float32, -1.5, 1.5))
    return (base * spread).reshape(SEQS, D).astype(jnp.bfloat16)


def draw_out_proj(key, part):
    subkeys = jax.random.split(jax.random.fold_in(key, 23), 2)
    base = jnp.clip(jax.random.normal(subkeys[0], (H * DV, D), jnp.float32), -4.0, 4.0)
    spread = jnp.exp(jax.random.uniform(subkeys[1], (1, D), jnp.float32, -1.5, 1.5))
    return (base * spread / jnp.sqrt(jnp.float32(H * DV))).astype(jnp.bfloat16)


def shard_levels(own_key, extent, cuts, least, high):
    level, own = 1.0, jax.random.fold_in(own_key, 6)
    for dim, parts in cuts:
        steps = jnp.exp(jax.random.uniform(jax.random.fold_in(own, dim), (parts,), jnp.float32, least / len(cuts), high / len(cuts)))
        level = level * jnp.repeat(steps, extent[dim] // parts).reshape([-1 if axis == dim else 1 for axis in range(len(extent))])
    return level


def centred(rng, dims, width, bound, pieces=(), kind=jnp.bfloat16):
    loudness = shard_levels(rng, dims, pieces, -0.22, 0.18) if pieces else 1.0
    values = jax.random.normal(rng, dims, jnp.float32) * width * loudness
    return jnp.minimum(jnp.maximum(values, -bound), bound).astype(kind)


def setup_inputs(seed: int = 0) -> dict:
    seeds = jax.random.split(jax.random.key(seed), 17)
    return {
        "hidden_in": draw_hidden_in(jax.random.fold_in(seeds[16], 71), 0),
        "input_gain": jnp.clip(1.0 + 0.18 * jax.random.normal(seeds[1], (D,), jnp.float32), 0.1, 1.9),
        "down_query": centred(seeds[2], (D, QR), D ** -0.5, 0.1875, ((0, 8),)),
        "down_latent": centred(seeds[3], (D, KR), D ** -0.5, 0.1875, ((0, 8),)),
        "down_rope": centred(seeds[4], (D, DR), D ** -0.5, 0.1875, ((0, 8),)),
        "query_gain": jnp.clip(1.0 + 0.18 * jax.random.normal(seeds[5], (QR,), jnp.float32), 0.1, 1.9),
        "latent_gain": jnp.clip(1.0 + 0.18 * jax.random.normal(seeds[6], (KR,), jnp.float32), 0.1, 1.9),
        "up_query": centred(seeds[7], (QR, H, DN), QR ** -0.5, 0.375, ((1, 8),)),
        "up_rope": centred(seeds[8], (QR, H, DR), QR ** -0.5, 0.375, ((1, 8),)),
        "key_up": centred(seeds[9], (KR, H, DN), KR ** -0.5, 0.375, ((1, 8),)),
        "value_up": centred(seeds[10], (KR, H, DV), KR ** -0.5, 0.375, ((1, 8),)),
        "out_proj": draw_out_proj(jax.random.fold_in(seeds[16], 71), 0),
        "output_gain": jnp.clip(1.0 + 0.18 * jax.random.normal(seeds[12], (D,), jnp.float32), 0.1, 1.9),
        "latent_cache": centred(seeds[13], (SEQS, LEN, KR), 1.0, 6.0, ((1, 512),)),
        "rope_cache": centred(seeds[14], (SEQS, LEN, DR), 1.0, 6.0, ((1, 512),)),
        "lengths": draw_lengths(jax.random.fold_in(seeds[16], 71), 0),
    }


THETA = 10000.0
EPSILON = 1e-06

def rotate(values, angles):
    half_width = values.shape[-1] // 2
    first_half = values[..., :half_width]
    second_half = values[..., half_width:]
    cosine = jnp.cos(angles)
    sine_part = jnp.sin(angles)
    return jnp.concatenate([first_half * cosine - second_half * sine_part, second_half * cosine + first_half * sine_part], axis=-1)

def angles_for(positions, rot_width):
    inverse = 1.0 / THETA ** (jnp.arange(0, rot_width, 2, dtype=jnp.float32) / rot_width)
    return positions[:, None] * inverse[None, :]

def normed(values, gain_row):
    return values * lax.rsqrt(lax.optimization_barrier(jnp.mean(values * values, axis=-1, keepdims=True)) + EPSILON) * gain_row.astype(jnp.float32)

def widen(values):
    return values.astype(jnp.float32)

def settle(values):
    return lax.optimization_barrier(values.astype(jnp.bfloat16))

def reference(hidden_in, input_gain, down_query, down_latent, down_rope, query_gain, latent_gain, up_query, up_rope, key_up, value_up, out_proj, output_gain, latent_cache, rope_cache, lengths):
    floats = widen(hidden_in)
    inv_rms = lax.rsqrt(lax.optimization_barrier(jnp.mean(floats * floats, axis=1, keepdims=True)) + EPSILON)
    scaled = (floats * widen(input_gain)).astype(jnp.bfloat16)
    query_low = jnp.dot(scaled, down_query, preferred_element_type=jnp.float32) * inv_rms
    latent_low = jnp.dot(scaled, down_latent, preferred_element_type=jnp.float32) * inv_rms
    rope_low = jnp.dot(scaled, down_rope, preferred_element_type=jnp.float32) * inv_rms
    positions = lengths.astype(jnp.float32)
    query_normed = settle(normed(query_low, query_gain))
    query_nope = settle(jnp.einsum('bq,qhd->bhd', widen(query_normed), widen(up_query)))
    query_rope = jnp.einsum('bq,qhr->bhr', widen(query_normed), widen(up_rope))
    query_rope = settle(rotate(query_rope, angles_for(positions, DR)[:, None, :]))
    latent_query = settle(jnp.einsum('bhd,chd->bhc', widen(query_nope), widen(key_up)))
    latent_new = settle(normed(latent_low, latent_gain))
    rope_new = settle(rotate(rope_low, angles_for(positions, DR)))
    factor = 1.0 / math.sqrt(DN + DR)
    places = jnp.arange(LEN, dtype=jnp.int32)

    def one_sequence(inputs):
        seq_query, seq_rope, latents, rotated, fresh_latent, fresh_rope, length = inputs
        scores = (jnp.einsum('hc,pc->hp', widen(seq_query), widen(latents)) + jnp.einsum('hr,pr->hp', widen(seq_rope), widen(rotated))) * factor
        usable = places < length
        scores = jnp.where(usable[None, :], scores, -1e+30)
        new_score = (lax.optimization_barrier(jnp.sum(widen(seq_query) * widen(fresh_latent)[None, :], axis=-1)) + lax.optimization_barrier(jnp.sum(widen(seq_rope) * widen(fresh_rope)[None, :], axis=-1))) * factor
        highest = jnp.maximum(lax.optimization_barrier(jnp.max(scores, axis=-1)), new_score)
        weights = jnp.where(usable[None, :], jnp.exp(scores - highest[:, None]), 0.0)
        fresh_weight = jnp.exp(new_score - highest)
        total_mass = lax.optimization_barrier(jnp.sum(weights, axis=-1)) + fresh_weight
        summed = jnp.einsum('hp,pc->hc', widen(settle(weights)), widen(latents)) + fresh_weight[:, None] * widen(fresh_latent)[None, :]
        return summed / total_mass[:, None]
    attended = lax.map(one_sequence, (latent_query, query_rope, latent_cache, rope_cache, latent_new, rope_new, lengths))
    attended = settle(attended)
    values_out = settle(jnp.einsum('bhc,chv->bhv', widen(attended), widen(value_up)))
    flattened = values_out.reshape(values_out.shape[0], H * DV)
    out_full = jnp.dot(flattened, out_proj, preferred_element_type=jnp.float32)
    out_rms = lax.rsqrt(lax.optimization_barrier(jnp.mean(out_full * out_full, axis=1, keepdims=True)) + EPSILON)
    return (out_full * out_rms * widen(output_gain)).astype(jnp.bfloat16)
```

```python
import functools
import math

import jax
import jax.numpy as jnp
from jax import lax
from jax.experimental import pallas as pl
from jax.experimental.pallas import tpu as pltpu
from jax.sharding import Mesh
from jax.sharding import PartitionSpec as P

D = 1024
DN = 128
DR = 64
THETA = 10000.0
EPSILON = 1e-06
FACTOR = 1.0 / math.sqrt(DN + DR)
LOW = -1e30
TP = ("x", "c")
KV = ("z", "y")
KV_TP = ("z", "y", "x", "c")
MESH = pl.DeviceIdType.MESH
F32 = jnp.float32
BF16 = jnp.bfloat16

TP_ORDER = (4, 5, 2, 3, 6, 7, 1)
RING_ORDER = (4, 3, 5, 2, 6, 1, 7)


def mirrored(slot):
    dx, dc = slot // 2, slot % 2
    return ((4 - dx) % 4) * 2 + dc


def dot(a, b, dims):
    return lax.dot_general(a, b, (dims, ((), ())), preferred_element_type=F32)


def iota(shape, dim):
    return lax.broadcasted_iota(jnp.int32, shape, dim)


def cos_sin(angle):
    turns = jnp.floor(angle * (2.0 / math.pi) + 0.5)
    r = angle - turns * 1.5703125
    r = r - turns * 4.825592041015625e-4
    r = r - turns * 1.2675907950567e-6
    r2 = r * r
    sine = r + r * r2 * (-1 / 6 + r2 * (1 / 120 + r2 * (-1 / 5040 + r2 * (1 / 362880))))
    cosine = 1.0 + r2 * (
        -0.5 + r2 * (1 / 24 + r2 * (-1 / 720 + r2 * (1 / 40320 + r2 * (-1 / 3628800))))
    )
    quadrant = turns - 4.0 * jnp.floor(turns * 0.25)
    odd = (quadrant == 1.0) | (quadrant == 3.0)
    c = jnp.where(odd, sine, cosine)
    s = jnp.where(odd, cosine, sine)
    c = jnp.where((quadrant == 1.0) | (quadrant == 2.0), -c, c)
    s = jnp.where((quadrant == 2.0) | (quadrant == 3.0), -s, s)
    return c, s


def split_lanes(value, rows):
    wide = jnp.broadcast_to(value, (rows, 128))
    high = wide.astype(BF16).astype(F32)
    rest = wide - high
    mid = rest.astype(BF16).astype(F32)
    low = rest - mid
    lane = iota((rows, 128), 1)
    return jnp.where(lane < 32, high, jnp.where(lane < 64, mid, low)).astype(BF16)


def joined_lanes(block):
    wide = block.astype(F32)
    return wide[:, 0:1] + wide[:, 32:33] + wide[:, 64:65]


def merged(parts):
    top = parts[0][1]
    for _, lse in parts[1:]:
        top = jnp.maximum(top, lse)
    weights = [jnp.exp(lse - top) for _, lse in parts]
    mass = weights[0]
    for w in weights[1:]:
        mass = mass + w
    total = parts[0][0] * weights[0]
    for (values, _), w in zip(parts[1:], weights[1:]):
        total = total + values * w
    return total * (1.0 / mass), top + jnp.log(mass)


def kernel(
    lengths,
    hidden_h, igain_h, dq_h, dl_h, dr_h, qgain_h, lgain_h, uq_h, ur_h, ku_h, vu_h, op_h, ogain_h, lat_h, rop_h,
    out,
    hidden, igain, dq, dl, dr, qgain, lgain, uq, ur, ku, vu, ogain, lat, rop,
    s1, r1, s1b, r1b, s2, r2, s3, r3, s4, r4, s5, r5, s6, r6, wt,
    load_sem, send_sem, recv_sem,
):
    z, y, x, c = (lax.axis_index(a) for a in KV_TP)
    me = x * 2 + c

    def tp_peer(slot):
        dx, dc = slot // 2, slot % 2
        return {"x": lax.rem(x + dx, 4), "c": lax.rem(c + dc, 2)}

    def y_peer(d):
        return {"y": lax.rem(y + d, 8)}

    def z_peer(d):
        return {"z": lax.rem(z + d, 8)}

    barrier = pltpu.get_barrier_semaphore()
    for slot in TP_ORDER:
        pl.semaphore_signal(barrier, inc=1, device_id=tp_peer(slot), device_id_type=MESH)
    for d in RING_ORDER:
        pl.semaphore_signal(barrier, inc=1, device_id=y_peer(d), device_id_type=MESH)
        pl.semaphore_signal(barrier, inc=1, device_id=z_peer(d), device_id_type=MESH)

    pairs = (
        (hidden_h, hidden), (igain_h, igain), (dq_h, dq), (dl_h, dl), (dr_h, dr), (op_h, wt.at[0, 0]),
        (qgain_h, qgain), (lgain_h, lgain), (uq_h, uq), (ur_h, ur), (ku_h, ku), (lat_h, lat), (rop_h, rop),
        (vu_h, vu), (ogain_h, ogain),
    )
    loads = {}
    for i, (src, dst) in enumerate(pairs):
        loads[i] = pltpu.make_async_copy(src, dst, load_sem.at[i])
        loads[i].start()

    sent = []

    def copy(phase, src, dst, send_slot, recv_slot, peer):
        return pltpu.make_async_remote_copy(
            src_ref=src,
            dst_ref=dst,
            send_sem=send_sem.at[phase, send_slot],
            recv_sem=recv_sem.at[phase, recv_slot],
            device_id=peer,
            device_id_type=MESH,
        )

    def tp_start(phase, src, dst):
        for slot in TP_ORDER:
            there = mirrored(slot)
            one = copy(phase, src(slot), dst(there), slot, there, tp_peer(slot))
            one.start()
            sent.append(one)

    def ring_start(phase, src, dst, peer):
        for d in RING_ORDER:
            there = 8 - d
            one = copy(phase, src, dst(there), d, there, peer(d))
            one.start()
            sent.append(one)

    def wait(phase, dst, order):
        for slot in order:
            copy(phase, dst(slot), dst(slot), slot, slot, tp_peer(1)).wait_recv()

    for i in (0, 1, 2):
        loads[i].wait()
    floats = hidden[...].astype(F32)
    scaled = (floats * igain[...]).astype(BF16)
    square = jnp.sum(floats * floats, axis=1, keepdims=True)
    s1[:, 0:256] = dot(scaled, dq[...], ((1,), (0,))).astype(BF16)
    s1[:, 256:384] = split_lanes(square, 8)
    for i in (3, 4):
        loads[i].wait()
    s1b[:, 0:256] = dot(scaled, dl[...], ((1,), (0,))).astype(BF16)
    rope_down = jnp.concatenate([dr[...], dr[...]], axis=0)
    s1b[:, 256:384] = dot(scaled, rope_down, ((1,), (1,))).astype(BF16)
    loads[5].wait()

    row = iota((8, 128), 0)
    lane = iota((8, 128), 1)
    length = jnp.zeros((8, 128), jnp.int32)
    for b in range(8):
        length = jnp.where(row == b, lengths[b], length)
    frequency = jnp.zeros((8, 128), F32)
    within = lax.rem(lane, 32)
    for i in range(32):
        frequency = jnp.where(within == i, float(THETA ** (-2.0 * i / DR)), frequency)
    cosine, sine = cos_sin(length.astype(F32) * frequency)
    sine = jnp.where(lax.rem(lane, 64) < 32, -sine, sine)

    def rotated(doubled):
        return doubled * cosine + pltpu.roll(doubled, 32, 1) * sine

    pl.semaphore_wait(barrier, 21)
    tp_start(0, lambda slot: s1, lambda slot: r1.at[slot])
    tp_start(1, lambda slot: s1b, lambda slot: r1b.at[slot])
    ring_start(2, wt.at[0, 0], lambda d: wt.at[0, d], y_peer)

    r1[0] = s1[...]
    r1b[0] = s1b[...]
    for i in (6, 7, 8, 9, 10):
        loads[i].wait()
    wait(0, lambda slot: r1.at[slot], TP_ORDER[::-1])
    total = r1[0, :, 0:384].astype(F32)
    for slot in range(1, 8):
        total = total + r1[slot].astype(F32)
    inv_rms = lax.rsqrt(joined_lanes(total[:, 256:384]) / D + EPSILON)

    def normed(values, gain):
        return values * lax.rsqrt(jnp.mean(values * values, axis=1, keepdims=True) + EPSILON) * gain

    query = normed(total[:, 0:256] * inv_rms, qgain[...]).astype(BF16)
    nope = dot(query, uq[...], ((1,), (0,))).astype(BF16)
    rope_up = jnp.concatenate([ur[...], ur[...]], axis=0)
    rope = rotated(dot(query, rope_up, ((1,), (1,)))).astype(BF16)
    latent = dot(nope, ku[...], ((1,), (1,))).astype(BF16)
    s2[:, 0:256] = latent
    s2[:, 256:384] = rope
    tp_start(3, lambda slot: s2, lambda slot: r2.at[slot])
    r2[0] = s2[...]

    wait(1, lambda slot: r1b.at[slot], TP_ORDER[::-1])
    fresh = r1b[0].astype(F32)
    for slot in range(1, 8):
        fresh = fresh + r1b[slot].astype(F32)
    fresh = fresh * inv_rms
    latent_new = normed(fresh[:, 0:256], lgain[...]).astype(BF16).astype(F32)
    rope_new = rotated(fresh[:, 256:384]).astype(BF16).astype(F32)
    new_score = jnp.sum(latent.astype(F32) * latent_new, axis=1, keepdims=True)
    new_score = new_score + jnp.sum(
        jnp.where(lane < 64, rope.astype(F32) * rope_new, 0.0), axis=1, keepdims=True
    )
    first_row = (z + y) == 0
    new_score = jnp.where(first_row, new_score * FACTOR, LOW)
    wait(2, lambda d: wt.at[0, d], RING_ORDER[::-1])
    ring_start(4, wt.at[0], lambda d: wt.at[d], z_peer)
    for i in (11, 12, 13, 14):
        loads[i].wait()

    wait(3, lambda slot: r2.at[slot], TP_ORDER[::-1])
    queries = r2[...].reshape(64, 384)
    keys = lat[...].reshape(1024, 256)
    rope_keys = jnp.concatenate([rop[b] for b in range(8)], axis=1)
    every = dot(queries[:, 0:256], keys, ((1,), (1,))) + dot(queries[:, 256:320], rope_keys, ((1,), (0,)))
    row64 = lax.rem(iota((64, 128), 0), 8)
    scores = every[:, 0:128]
    for b in range(1, 8):
        scores = jnp.where(row64 == b, every[:, b * 128 : (b + 1) * 128], scores)
    place = ((z * 8 + y) * 8 + me) * 128 + iota((64, 128), 1)
    usable = place < jnp.concatenate([length] * 8, axis=0)
    scores = jnp.where(usable, scores * FACTOR, LOW)
    top = jnp.max(scores, axis=1, keepdims=True)
    weights = jnp.where(usable, jnp.exp(scores - top), 0.0)
    mass = jnp.sum(weights, axis=1, keepdims=True)
    spread = jnp.concatenate([jnp.where(row64 == b, weights, 0.0).astype(BF16) for b in range(8)], axis=1)
    summed = dot(spread, keys, ((1,), (0,)))
    some = mass > 0.0
    safe = jnp.where(some, mass, 1.0)
    summed = summed * (1.0 / safe)
    lse = jnp.where(some, top + jnp.log(safe), LOW)
    split = split_lanes(lse, 64)
    for slot in range(8):
        s3[slot, :, 0:256] = summed[slot * 8 : slot * 8 + 8].astype(BF16)
        s3[slot, :, 256:384] = split[slot * 8 : slot * 8 + 8]
    tp_start(5, lambda slot: s3.at[slot], lambda slot: r3.at[slot])
    r3[0] = s3[0]

    wait(5, lambda slot: r3.at[slot], TP_ORDER[::-1])
    parts = [(latent_new, new_score)]
    for slot in range(8):
        parts.append((r3[slot, :, 0:256].astype(F32), joined_lanes(r3[slot, :, 256:384])))
    attended, lse = merged(parts)
    values = dot(attended.astype(BF16), vu[...], ((1,), (0,)))

    def ring_merge(phase, values, lse, send, recv, peer):
        send[:, 0:128] = values.astype(BF16)
        send[:, 128:256] = split_lanes(lse, 8)
        ring_start(phase, send, lambda d: recv.at[d], peer)
        recv[0] = send[...]
        wait(phase, lambda d: recv.at[d], RING_ORDER[::-1])
        return merged([(recv[d, :, 0:128].astype(F32), joined_lanes(recv[d, :, 128:256])) for d in range(8)])

    values, lse = ring_merge(6, values, lse, s4, r4, y_peer)
    values, lse = ring_merge(7, values, lse, s5, r5, z_peer)

    wait(4, lambda d: wt.at[d], RING_ORDER[::-1])
    columns = wt[...].reshape(1024, 128)
    s6[...] = dot(values.astype(BF16), columns, ((1,), (1,))).astype(BF16)
    for slot in TP_ORDER:
        one = copy(8, s6, r6.at[me], slot, mirrored(slot), tp_peer(slot))
        one.start()
        sent.append(one)
    r6[me] = s6[...]
    for slot in TP_ORDER[::-1]:
        copy(8, s6, r6.at[0], slot, slot, tp_peer(1)).wait_recv()
    full = r6[0].astype(F32)
    for h in range(1, 8):
        full = full + r6[h].astype(F32)
    rms = lax.rsqrt(jnp.sum(full * full, axis=1, keepdims=True) / D + EPSILON)
    out[...] = (full[:, 0:16] * rms * ogain[...]).astype(BF16)
    for one in sent:
        one.wait_send()


def body(
    hidden_in, input_gain, down_query, down_latent, down_rope, query_gain, latent_gain, up_query, up_rope,
    key_up, value_up, out_proj, output_gain, latent_cache, rope_cache, lengths,
):
    operands = (
        hidden_in,
        input_gain.reshape(1, 128),
        down_query,
        down_latent,
        down_rope.T,
        query_gain.reshape(1, 256),
        latent_gain.reshape(1, 256),
        up_query.transpose(1, 0, 2).reshape(256, 128),
        up_rope.transpose(1, 2, 0).reshape(64, 256),
        key_up.transpose(1, 0, 2).reshape(256, 128),
        value_up.transpose(1, 0, 2).reshape(256, 128),
        out_proj.T,
        output_gain.reshape(1, 16),
        latent_cache,
        rope_cache.transpose(0, 2, 1),
    )
    loaded = [pltpu.VMEM(a.shape, a.dtype) for i, a in enumerate(operands) if i != 11]
    message = lambda *shape: pltpu.VMEM(shape, BF16)
    return pl.pallas_call(
        kernel,
        out_shape=jax.ShapeDtypeStruct((8, 16), BF16),
        in_specs=[pl.BlockSpec(memory_space=pltpu.SMEM)] + [pl.BlockSpec(memory_space=pl.ANY)] * len(operands),
        out_specs=pl.BlockSpec(memory_space=pltpu.VMEM),
        scratch_shapes=[
            *loaded,
            message(8, 384), message(8, 8, 384),
            message(8, 384), message(8, 8, 384),
            message(8, 384), message(8, 8, 384),
            message(8, 8, 384), message(8, 8, 384),
            message(8, 256), message(8, 8, 256),
            message(8, 256), message(8, 8, 256),
            message(8, 1024), message(8, 8, 1024),
            message(8, 8, 16, 128),
            pltpu.SemaphoreType.DMA((15,)),
            pltpu.SemaphoreType.DMA((9, 8)),
            pltpu.SemaphoreType.DMA((9, 8)),
        ],
        compiler_params=pltpu.CompilerParams(collective_id=0, has_side_effects=True),
    )(lengths, *operands)


def solution(mesh):
    split = Mesh(mesh.devices.reshape(8, 8, 4, 2), KV_TP)
    in_specs = (
        P(None, TP),
        P(TP),
        P(TP, None),
        P(TP, None),
        P(TP, None),
        P(),
        P(),
        P(None, TP, None),
        P(None, TP, None),
        P(None, TP, None),
        P(None, TP, None),
        P(TP, KV),
        P(KV),
        P(None, KV_TP, None),
        P(None, KV_TP, None),
        P(),
    )
    return jax.shard_map(body, mesh=split, in_specs=in_specs, out_specs=P(None, KV), check_vma=False)
```
